32 devices in a mesh: grp: 2 (over y), sp: 4 (over z), tp: 4 (over x, core).
Axes of the slice: x: 2, y: 2, z: 4, core: 2. Of those that a mesh axis runs over, the one named last changes fastest.
Arguments:
- latent: bfloat16 [4096, 4096], P(('grp', 'sp'), 'tp'), parts along dimension 0, may hold values from -42 to 42
- context: bfloat16 [2048, 4096], P(('grp', 'sp'), 'tp'), parts along dimension 0, may hold values from -42 to 42
- conditions: float32 [4, 4096], P('grp', 'sp'), parts along dimension 0, may hold values from -6 to 6
- mod_weight: bfloat16 [4096, 3, 4096], P('sp', None, 'tp'), may hold values from -0.09375 to 0.09375
- norm_gain: float32 [4096], P('tp'), may hold values from 0.1 to 1.9
- w_query: bfloat16 [4096, 2048], P(None, 'tp'), may hold values from -0.09375 to 0.09375
- w_key: bfloat16 [4096, 2048], P(None, 'tp'), may hold values from -0.09375 to 0.09375
- w_value: bfloat16 [4096, 2048], P(None, 'tp'), may hold values from -0.09375 to 0.09375
- query_gain: float32 [64], replicated, may hold values from 1 to 14
- key_gain: float32 [64], replicated, may hold values from 1 to 14
- lambdas: float32 [16], P('tp'), may hold values from 0.3 to 0.8
- out_gain: float32 [128], replicated, may hold values from 0.1 to 1.9
- w_out: bfloat16 [2048, 4096], P(None, 'tp'), may hold values from -0.125 to 0.125
Outputs:
- updated: bfloat16 [4096, 4096], P(('grp', 'sp'), 'tp'), parts along dimension 0
The draws below stay inside these ranges and needn't reach their ends.
There are 2 independent parts, one for each index of `grp`. The reference program is written for one: setup_inputs(seed, part) draws one part's arguments, and reference() takes and returns one part's arrays. A program takes and returns all parts, laid end to end along the dimension named above; an argument that names none is the same for every part. Nothing has to cross between parts.
All inputs are finite; a program needn't handle non-finite values.
Results may differ from the reference program's by a relative error of at most 0.0076.
Values may be sent and summed in bfloat16 or wider, within the bound.
A program may use at most 128 MiB of HBM per device.

```python
import math
import jax
import jax.numpy as jnp
from jax import lax

D = 4096
HEADS = 16
DK = 64
DV = 128
GRID_W = 64
CTX = 1024
LAT = 2048


def rising_rows(key, row_count):
    column = jnp.arange(D, dtype=jnp.float32)
    base = jnp.clip(jax.random.normal(key, (row_count, D), jnp.float32), -6.0, 6.0)
    return base * (1.0 + 2.0 * column / (D - 1))


def spiked_gains(key, which):
    own_key = jax.random.fold_in(key, which)
    return jax.random.uniform(own_key, (DK,), jnp.float32, 1.1, 1.5)


def draw_latent(key, part):
    return rising_rows(jax.random.fold_in(key, 21), LAT).astype(jnp.bfloat16)


def draw_context(key, part):
    return rising_rows(jax.random.fold_in(key, 22), CTX).astype(jnp.bfloat16)


def draw_query_gain(key, part):
    return spiked_gains(key, 1)


def draw_key_gain(key, part):
    return spiked_gains(key, 2)


def shard_levels(key, extent, pieces, smallest, high):
    loudness = 1.0
    for dim, parts in pieces:
        heights = jax.random.uniform(jax.random.fold_in(jax.random.fold_in(key, 6), dim), (parts,), jnp.float32, smallest / len(pieces), high / len(pieces))
        loudness = loudness * jnp.repeat(jnp.exp(heights), extent[dim] // parts).reshape((-1,) + (1,) * (len(extent) - 1 - dim))
    return loudness


def bell_draw(key, dims, deviation, most, shards=(), kind=jnp.bfloat16):
    result = deviation * jax.random.normal(key, dims, jnp.float32)
    if shards:
        result = result * shard_levels(key, dims, shards, -0.22, 0.18)
    return jnp.clip(result, -most, most).astype(kind)


def setup_inputs(seed: int = 0, part: int = 0) -> dict:
    keys = jax.random.split(jax.random.key(seed), 14)
    own_keys = jax.random.split(jax.random.fold_in(keys[13], part), 14)
    latent = draw_latent(jax.random.fold_in(jax.random.fold_in(keys[13], part), 71), part)
    context = draw_context(jax.random.fold_in(jax.random.fold_in(keys[13], part), 71), part)
    conditions = bell_draw(own_keys[2], (2, D), 1.0, 6.0, ((1, 4),), jnp.float32)
    mod_weight = bell_draw(keys[3], (D, 3, D), D ** -0.5, 0.09375, ((0, 4), (2, 4)))
    norm_gain = jnp.clip(1.0 + 0.18 * jax.random.normal(keys[4], (D,), jnp.float32), 0.1, 1.9)
    w_query = bell_draw(keys[5], (D, HEADS * 2 * DK), D ** -0.5, 0.09375, ((1, 4),))
    w_key = bell_draw(keys[6], (D, HEADS * 2 * DK), D ** -0.5, 0.09375, ((1, 4),))
    w_value = bell_draw(keys[7], (D, HEADS * DV), D ** -0.5, 0.09375, ((1, 4),))
    query_gain = draw_query_gain(jax.random.fold_in(keys[13], 71), part)
    key_gain = draw_key_gain(jax.random.fold_in(keys[13], 71), part)
    lambdas = jnp.clip(0.3 + 0.5 * jax.random.uniform(keys[10], (HEADS,), jnp.float32) ** shard_levels(keys[10], (HEADS,), ((0, 4),), -0.2, 0.2), 0.3, 0.8)
    out_gain = jnp.clip(1.0 + 0.18 * jax.random.normal(keys[11], (DV,), jnp.float32), 0.1, 1.9)
    w_out = bell_draw(keys[12], (HEADS * DV, D), (HEADS * DV) ** -0.5, 0.125, ((1, 4),))
    return {"latent": latent, "context": context, "conditions": conditions, "mod_weight": mod_weight, "norm_gain": norm_gain, "w_query": w_query, "w_key": w_key, "w_value": w_value, "query_gain": query_gain, "key_gain": key_gain, "lambdas": lambdas, "out_gain": out_gain, "w_out": w_out}


epsilon = 1e-06

def turn_half(halves, angles):
    quarter = halves.shape[-1] // 2
    cosine = jnp.cos(angles)[:, None, None, :]
    sine_part = jnp.sin(angles)[:, None, None, :]
    first_part = halves[..., :quarter]
    second = halves[..., quarter:]
    return jnp.concatenate([first_part * cosine - second * sine_part, first_part * sine_part + second * cosine], axis=-1)

def rotate(features, positions):
    half_width = features.shape[-1] // 2
    quarter = half_width // 2
    inverse = 10000.0 ** (-2.0 * jnp.arange(quarter, dtype=jnp.float32) / half_width)
    grid_row = (positions // GRID_W).astype(jnp.float32)
    grid_column = (positions % GRID_W).astype(jnp.float32)
    return jnp.concatenate([turn_half(features[..., :half_width], grid_row[:, None] * inverse), turn_half(features[..., half_width:], grid_column[:, None] * inverse)], axis=-1)

def head_norm(features, gain_row):
    return features * lax.rsqrt(lax.optimization_barrier(jnp.mean(features * features, axis=-1, keepdims=True)) + epsilon) * gain_row

def modulate(rows_in, gain_row, shift_row, scale_row):
    floats = rows_in.astype(jnp.float32)
    factor = lax.rsqrt(lax.optimization_barrier(jnp.mean(floats * floats, axis=1, keepdims=True)) + epsilon)
    return (floats * factor * gain_row * (1.0 + scale_row) + shift_row).astype(jnp.bfloat16)

def reference(latent, context, conditions, mod_weight, norm_gain, w_query, w_key, w_value, query_gain, key_gain, lambdas, out_gain, w_out):
    activated = jax.nn.silu(conditions).astype(jnp.bfloat16)
    modulation = jnp.dot(activated, mod_weight.reshape(D, 3 * D), preferred_element_type=jnp.float32).reshape(2, 3, D)
    hidden = modulate(latent, norm_gain, modulation[0, 0], modulation[0, 1])
    hidden_ctx = modulate(context, norm_gain, modulation[1, 0], modulation[1, 1])
    positions = jnp.arange(LAT, dtype=jnp.int32)
    query_raw = jnp.dot(hidden, w_query, preferred_element_type=jnp.float32).reshape(LAT, HEADS, 2, DK)
    key_raw = jnp.dot(hidden, w_key, preferred_element_type=jnp.float32).reshape(LAT, HEADS, 2, DK)
    ctx_key_raw = jnp.dot(hidden_ctx, w_key, preferred_element_type=jnp.float32).reshape(CTX, HEADS, 2, DK)
    queries = rotate(head_norm(query_raw, query_gain), positions).astype(jnp.bfloat16)
    lat_keys = rotate(head_norm(key_raw, key_gain), positions).astype(jnp.bfloat16)
    ctx_keys = head_norm(ctx_key_raw, key_gain).astype(jnp.bfloat16)
    lat_values = jnp.dot(hidden, w_value, preferred_element_type=jnp.float32).astype(jnp.bfloat16).reshape(LAT, HEADS, DV)
    ctx_values = jnp.dot(hidden_ctx, w_value, preferred_element_type=jnp.float32).astype(jnp.bfloat16).reshape(CTX, HEADS, DV)
    all_keys = jnp.concatenate([ctx_keys, lat_keys], axis=0)
    all_values = jnp.concatenate([ctx_values, lat_values], axis=0)
    block_rows = math.gcd(LAT, 512)
    scaling = DK ** (-0.5)

    def one_head(head_index):
        head_keys = lax.dynamic_index_in_dim(all_keys, head_index, 1, False).astype(jnp.float32)
        head_values = lax.dynamic_index_in_dim(all_values, head_index, 1, False).astype(jnp.float32)
        head_queries = lax.dynamic_index_in_dim(queries, head_index, 1, False).astype(jnp.float32)
        head_queries = head_queries.reshape(LAT // block_rows, block_rows, 2, DK)
        weight_lambda = lax.dynamic_index_in_dim(lambdas, head_index, 0, False)

        def one_block(query_block):
            scores = jnp.einsum('qmd,kmd->qmk', query_block, head_keys) * scaling
            row_peak = lax.optimization_barrier(jnp.max(scores, axis=-1, keepdims=True))
            exponent = jnp.exp(scores - row_peak)
            row_sums = lax.optimization_barrier(jnp.sum(exponent, axis=-1))
            weights = lax.optimization_barrier(exponent.astype(jnp.bfloat16)).astype(jnp.float32)
            blended = jnp.einsum('qmk,kv->qmv', weights, head_values)
            attended = blended[:, 0] / row_sums[:, 0, None] - weight_lambda * blended[:, 1] / row_sums[:, 1, None]
            return head_norm(attended, out_gain)
        return lax.map(one_block, head_queries).reshape(LAT, DV)
    outputs = lax.map(one_head, jnp.arange(HEADS, dtype=jnp.int32))
    head_out = jnp.transpose(outputs, (1, 0, 2)).reshape(LAT, HEADS * DV).astype(jnp.bfloat16)
    mixed_rows = jnp.dot(head_out, w_out, preferred_element_type=jnp.float32)
    return (latent.astype(jnp.float32) + modulation[0, 2] * mixed_rows).astype(jnp.bfloat16)
```

```python
import functools
import math

import jax
import jax.numpy as jnp
from jax import lax
from jax.experimental import pallas as pl
from jax.experimental.pallas import tpu as pltpu
from jax.sharding import PartitionSpec as P

DK = 64
DV = 128
GRID_W = 64


epsilon = 1e-06


def turn_half(halves, angles):
    quarter = halves.shape[-1] // 2
    cosine = jnp.cos(angles)[:, None, None, :]
    sine_part = jnp.sin(angles)[:, None, None, :]
    first_part = halves[..., :quarter]
    second = halves[..., quarter:]
    return jnp.concatenate(
        [first_part * cosine - second * sine_part, first_part * sine_part + second * cosine],
        axis=-1,
    )


def rotate(features, positions):
    half_width = features.shape[-1] // 2
    quarter = half_width // 2
    inverse = 10000.0 ** (-2.0 * jnp.arange(quarter, dtype=jnp.float32) / half_width)
    grid_row = (positions // GRID_W).astype(jnp.float32)
    grid_column = (positions % GRID_W).astype(jnp.float32)
    return jnp.concatenate(
        [
            turn_half(features[..., :half_width], grid_row[:, None] * inverse),
            turn_half(features[..., half_width:], grid_column[:, None] * inverse),
        ],
        axis=-1,
    )


def head_norm(features, gain_row):
    return (
        features
        * lax.rsqrt(jnp.mean(features * features, axis=-1, keepdims=True) + epsilon)
        * gain_row
    )


def modulate(rows_in, gain_row, shift_row, scale_row):
    floats = rows_in.astype(jnp.float32)
    factor = lax.rsqrt(jnp.mean(floats * floats, axis=1, keepdims=True) + epsilon)
    return (floats * factor * gain_row * (1.0 + scale_row) + shift_row).astype(jnp.bfloat16)


def plain(
    latent,
    context,
    conditions,
    mod_weight,
    norm_gain,
    w_query,
    w_key,
    w_value,
    query_gain,
    key_gain,
    lambdas,
    out_gain,
    w_out,
):
    tok_rows = latent.shape[0]
    ctx_rows = context.shape[0]
    columns = latent.shape[1]
    heads_here = lambdas.shape[0]
    in_rows = mod_weight.shape[0]
    activated = jax.nn.silu(conditions).astype(jnp.bfloat16)
    partial_mod = jnp.dot(
        activated, mod_weight.reshape(in_rows, 3 * columns), preferred_element_type=jnp.float32
    ).reshape(2, 3, columns)
    modulation = lax.psum(partial_mod, "sp")
    lat_floats = latent.astype(jnp.float32)
    full_gain, full_pairs = (
        lax.all_gather(norm_gain, "tp", axis=0, tiled=True),
        lax.all_gather(modulation[:, :2], "tp", axis=2, tiled=True),
    )
    whole_lat, whole_ctx = (
        lax.all_gather(latent, "tp", axis=1, tiled=True),
        lax.all_gather(context, "tp", axis=1, tiled=True),
    )
    hidden = modulate(whole_lat, full_gain, full_pairs[0, 0], full_pairs[0, 1])
    hidden_ctx = modulate(whole_ctx, full_gain, full_pairs[1, 0], full_pairs[1, 1])
    query_raw = jnp.dot(hidden, w_query, preferred_element_type=jnp.float32)
    key_raw = jnp.dot(hidden, w_key, preferred_element_type=jnp.float32)
    value_raw = jnp.dot(hidden, w_value, preferred_element_type=jnp.float32)
    ctx_key_raw = jnp.dot(hidden_ctx, w_key, preferred_element_type=jnp.float32)
    ctx_value_raw = jnp.dot(hidden_ctx, w_value, preferred_element_type=jnp.float32)
    positions = lax.axis_index("sp") * tok_rows + jnp.arange(tok_rows, dtype=jnp.int32)
    queries = rotate(
        head_norm(query_raw.reshape(tok_rows, heads_here, 2, DK), query_gain), positions
    ).astype(jnp.bfloat16)
    lat_keys = (
        rotate(head_norm(key_raw.reshape(tok_rows, heads_here, 2, DK), key_gain), positions)
        .astype(jnp.bfloat16)
        .reshape(tok_rows, heads_here * 2 * DK)
    )
    lat_values = value_raw.astype(jnp.bfloat16)
    ctx_keys = (
        head_norm(ctx_key_raw.reshape(ctx_rows, heads_here, 2, DK), key_gain)
        .astype(jnp.bfloat16)
        .reshape(ctx_rows, heads_here * 2 * DK)
    )
    ctx_values = ctx_value_raw.astype(jnp.bfloat16)
    scaling = DK ** (-0.5)

    def absorb(carried, key_rows, value_rows):
        key_count = key_rows.shape[0]
        key_block = key_rows.reshape(key_count, heads_here, 2, DK)
        value_block = value_rows.reshape(key_count, heads_here, DV)
        running_max, totals, weighted = carried
        scores = (
            jnp.einsum("qhmd,khmd->qhmk", queries, key_block, preferred_element_type=jnp.float32)
            * scaling
        )
        new_max = jnp.maximum(running_max, jnp.max(scores, axis=-1))
        rescale = jnp.exp(running_max - new_max)
        exponent = jnp.exp(scores - new_max[..., None])
        totals = totals * rescale + jnp.sum(exponent, axis=-1)
        weighted = weighted * rescale[..., None] + jnp.einsum(
            "qhmk,khv->qhmv",
            exponent.astype(jnp.bfloat16),
            value_block,
            preferred_element_type=jnp.float32,
        )
        return (new_max, totals, weighted)

    def absorb_rows(carried, key_rows, value_rows):
        key_count = key_rows.shape[0]
        block_rows = math.gcd(key_count, 512)

        def visit_block(block_index, partial_value):
            first_row = block_index * block_rows
            return absorb(
                partial_value,
                lax.dynamic_slice_in_dim(key_rows, first_row, block_rows, 0),
                lax.dynamic_slice_in_dim(value_rows, first_row, block_rows, 0),
            )

        return lax.fori_loop(0, key_count // block_rows, visit_block, carried)

    initial_state = (
        jnp.full((tok_rows, heads_here, 2), -1e30, jnp.float32),
        jnp.zeros((tok_rows, heads_here, 2), jnp.float32),
        jnp.zeros((tok_rows, heads_here, 2, DV), jnp.float32),
    )
    every_ctx_keys, every_ctx_values = (
        lax.all_gather(ctx_keys, "sp", axis=0, tiled=True),
        lax.all_gather(ctx_values, "sp", axis=0, tiled=True),
    )
    carried = absorb_rows(initial_state, every_ctx_keys, every_ctx_values)
    carried = absorb_rows(
        carried,
        lax.all_gather(lat_keys, "sp", axis=0, tiled=True),
        lax.all_gather(lat_values, "sp", axis=0, tiled=True),
    )
    running_max, totals, weighted = carried
    attended = (
        weighted[:, :, 0] / totals[:, :, 0, None]
        - lambdas[None, :, None] * weighted[:, :, 1] / totals[:, :, 1, None]
    )
    head_out = head_norm(attended, out_gain).astype(jnp.bfloat16).reshape(tok_rows, heads_here * DV)
    mixed_rows = jnp.dot(
        lax.all_gather(head_out, "tp", axis=1, tiled=True),
        w_out,
        preferred_element_type=jnp.float32,
    )
    return (lat_floats + modulation[0, 2] * mixed_rows).astype(jnp.bfloat16)


MESH = pl.DeviceIdType.MESH
BF = jnp.bfloat16
F32 = jnp.float32


def fused_kernel(
    sp, tp, lat, ctx, part, gain, wq_h, wk_h, wv_h, wo_h, qc, qs, kc, ks, ckg, lam, og, ones_bd,
    out, X, PA, CO, WQ, WK, WV, WO, H, SL, SC, RL, RC, KX, VX, SS, OS, HO,
    loc_sem, w_sem, xs, xr, ds, dr, fs, fr, ps, pr, cs, cr, zs, zr, os_, or_, gs, gr, es, er, hs, hr,
):
    ms = lax.axis_index("sp")
    mt = lax.axis_index("tp")
    nx = tp // 2
    core = lax.rem(mt, 2)
    base = mt - core
    mate = base + 1 - core
    xp = [lax.rem(base + 2 * d, tp) + core for d in range(1, nx)]
    xq = [lax.rem(base + tp - 2 * d, tp) + core for d in range(1, nx)]
    xqm = [lax.rem(base + tp - 2 * d, tp) + 1 - core for d in range(1, nx)]
    zp = [lax.rem(ms + d, sp) for d in range(1, sp)]
    zq = [lax.rem(ms + sp - d, sp) for d in range(1, sp)]
    tpn = [lax.rem(mt + d, tp) for d in range(1, tp)]
    tpq = [lax.rem(mt + tp - d, tp) for d in range(1, tp)]
    n = ctx.shape[0]
    cols = lat.shape[1]
    nl = lat.shape[0] // n

    barrier = pltpu.get_barrier_semaphore()
    for p in zp:
        pl.semaphore_signal(barrier, inc=1, device_id={"sp": p}, device_id_type=MESH)
    for p in tpn:
        pl.semaphore_signal(barrier, inc=1, device_id={"tp": p}, device_id_type=MESH)

    def local_in(c):
        src = ctx if c == 0 else lat.at[pl.ds((c - 1) * n, n)]
        return pltpu.make_async_copy(src, X.at[mt, pl.ds(c * n, n)], loc_sem.at[c])

    for c in range(nl + 1):
        local_in(c).start()
    weights = [
        pltpu.make_async_copy(a, b, w_sem.at[i])
        for i, (a, b) in enumerate(((wk_h, WK), (wv_h, WV), (wq_h, WQ), (wo_h, WO)))
    ]
    for w in weights:
        w.start()
    pl.semaphore_wait(barrier, (sp - 1) + (tp - 1))

    def remote(src, dst, ssem, rsem, where):
        return pltpu.make_async_remote_copy(
            src_ref=src, dst_ref=dst, send_sem=ssem, recv_sem=rsem,
            device_id=where, device_id_type=MESH,
        )

    def source(c):
        return ctx if c == 0 else lat.at[pl.ds((c - 1) * n, n)]

    def x_send(c, d):
        return remote(source(c), X.at[mt, pl.ds(c * n, n)], xs.at[c, d], xr.at[c, d], {"tp": xp[d]})

    def d_send(c):
        return remote(source(c), X.at[mt, pl.ds(c * n, n)], ds.at[c], dr.at[c], {"tp": mate})

    def p_send(d):
        return remote(part, PA.at[ms], ps.at[d], pr.at[d], {"sp": zp[d]})

    def c_send(d):
        return remote(CO.at[mt], CO.at[mt], cs.at[d], cr.at[d], {"tp": tpn[d]})

    for d in range(sp - 1):
        p_send(d).start()
    for d in range(nx - 1):
        x_send(0, d).start()
    for c in range(nl + 1):
        d_send(c).start()

    PA[ms] = part[...]
    for d in range(sp - 1):
        p_send(d).wait()
    total = PA[0]
    for s in range(1, sp):
        total = total + PA[s]
    CO[mt, 0:1, :] = gain[...] * (1.0 + total[1:2])
    CO[mt, 1:2, :] = total[0:1]
    CO[mt, 2:3, :] = gain[...] * (1.0 + total[4:5])
    CO[mt, 3:4, :] = total[3:4]
    CO[mt, 4:5, :] = total[2:3]
    CO[mt, 5:8, :] = jnp.zeros((3, cols), F32)
    for d in range(tp - 1):
        c_send(d).start()
    for c in range(1, nl + 1):
        for d in range(nx - 1):
            x_send(c, d).start()
    for d in range(tp - 1):
        c_send(d).wait()

    lane = lax.broadcasted_iota(jnp.int32, (n, 2 * DK), 1)
    low = lax.rem(lane, DK // 2) < DK // 4

    def f_send(c, d):
        ref = X.at[xq[d], pl.ds(c * n, n)]
        return remote(ref, ref, fs.at[c, d], fr.at[c, d], {"tp": mate})

    def z_send(c, d):
        if c == 0:
            return remote(SC.at[zp[d]], RC.at[ms], zs.at[c, d], zr.at[c, d], {"sp": zp[d]})
        return remote(
            SL.at[zp[d], c - 1], RL.at[ms, c - 1], zs.at[c, d], zr.at[c, d], {"sp": zp[d]}
        )

    def normed(v):
        square = (v * v).astype(BF)
        mean = jnp.dot(square, ones_bd[...], preferred_element_type=F32)
        return v * lax.rsqrt(mean * (1.0 / DK) + epsilon)

    def turned(v, ctab, stab):
        w = normed(v)
        swapped = jnp.where(low, pltpu.roll(w, 2 * DK - DK // 4, 1), pltpu.roll(w, DK // 4, 1))
        return (w * ctab + swapped * stab).astype(BF)

    for c in range(nl + 1):
        rows = pl.ds(c * n, n)
        local_in(c).wait()
        for d in range(nx - 1):
            x_send(c, d).wait()
            f_send(c, d).start()
        d_send(c).wait()
        for d in range(nx - 1):
            f_send(c, d).wait()
        ss = jnp.zeros((n, 1), F32)
        for t in range(tp):
            f = X[t, rows, :].astype(F32)
            ss = ss + jnp.sum(f * f, axis=1, keepdims=True)
        factor = lax.rsqrt(ss * (1.0 / (tp * cols)) + epsilon)
        r0 = 2 if c == 0 else 0
        for t in range(tp):
            f = X[t, rows, :].astype(F32)
            co = CO[t]
            H[:, t * cols:(t + 1) * cols] = (
                f * factor * co[r0:r0 + 1] + co[r0 + 1:r0 + 2]
            ).astype(BF)
        if c == 0:
            weights[0].wait()
            weights[1].wait()
        if c == 1:
            weights[2].wait()
        off = 0 if c == 0 else DV
        if c > 0:
            tr = pl.ds((c - 1) * n, n)
            raw = jnp.dot(H[...], WQ[...], preferred_element_type=F32)
            for z in range(sp):
                SL[z, c - 1, :, 0:DV] = turned(raw[:, z * DV:(z + 1) * DV], qc[tr, :], qs[tr, :])
        raw = jnp.dot(H[...], WK[...], preferred_element_type=F32)
        for z in range(sp):
            piece = raw[:, z * DV:(z + 1) * DV]
            if c == 0:
                SC[z, :, 0:DV] = (normed(piece) * ckg[...]).astype(BF)
            else:
                SL[z, c - 1, :, DV:2 * DV] = turned(piece, kc[tr, :], ks[tr, :])
        raw = jnp.dot(H[...], WV[...], preferred_element_type=F32)
        for z in range(sp):
            piece = raw[:, z * DV:(z + 1) * DV].astype(BF)
            if c == 0:
                SC[z, :, DV:2 * DV] = piece
            else:
                SL[z, c - 1, :, 2 * DV:3 * DV] = piece
        for d in range(sp - 1):
            z_send(c, d).start()
        if c == 0:
            RC[ms] = SC[ms]
        else:
            RL[ms, c - 1] = SL[ms, c - 1]

    for c in range(nl + 1):
        for d in range(sp - 1):
            z_send(c, d).wait()
    nk = sp * (nl + 1)
    for s in range(sp):
        for c in range(nl + 1):
            kb = s * (nl + 1) + c
            if c == 0:
                KX[kb] = RC[s, :, 0:DV]
                VX[kb, :, 0:DV] = RC[s, :, DV:2 * DV]
            else:
                KX[kb] = RL[s, c - 1, :, DV:2 * DV]
                VX[kb, :, 0:DV] = RL[s, c - 1, :, 2 * DV:3 * DV]
            VX[kb, :, DV:2 * DV] = jnp.ones((n, DV), BF)

    first = lane < DK

    def o_send(half, d):
        return remote(
            OS.at[half, zp[d]],
            HO.at[mt, pl.ds(half * n, n), pl.ds(pl.multiple_of(ms * DV, DV), DV)],
            os_.at[half, d], or_.at[half, d], {"sp": zp[d]},
        )

    def g_send(half, d):
        ref = HO.at[mt, pl.ds(half * n, n)]
        return remote(ref, ref, gs.at[half, d], gr.at[half, d], {"tp": xp[d]})

    def e_send(half):
        ref = HO.at[mt, pl.ds(half * n, n)]
        return remote(ref, ref, es.at[half], er.at[half], {"tp": mate})

    def h_send(half, d):
        ref = HO.at[xq[d], pl.ds(half * n, n)]
        return remote(ref, ref, hs.at[half, d], hr.at[half, d], {"tp": mate})

    def attend(z, half):
        q = RL[z, half, :, 0:DV]
        zero = jnp.zeros_like(q)
        qq = jnp.concatenate([jnp.where(first, q, zero), jnp.where(first, zero, q)], axis=0)
        peak = None
        for kb in range(nk):
            s = lax.dot_general(qq, KX[kb], (((1,), (1,)), ((), ())), preferred_element_type=F32)
            SS[kb] = s
            for j in range(n // 128):
                piece = s[:, j * 128:(j + 1) * 128]
                peak = piece if peak is None else jnp.maximum(peak, piece)
        peak = jnp.max(peak, axis=1, keepdims=True)
        acc = jnp.zeros((2 * n, 2 * DV), F32)
        for kb in range(nk):
            p = jnp.exp2(SS[kb] - peak).astype(BF)
            acc = acc + jnp.dot(p, VX[kb], preferred_element_type=F32)
        o = acc[:, :DV] / acc[:, DV:]
        a = o[:n] - lam[...] * o[n:]
        a = a * lax.rsqrt(jnp.mean(a * a, axis=1, keepdims=True) + epsilon) * og[...]
        return a.astype(BF)

    for half in range(nl):
        def step(i, carry):
            z = lax.rem(ms + 1 + i, sp)
            OS[half, z] = attend(z, half)
            for d in range(sp - 1):
                @pl.when(i == d)
                def _():
                    o_send(half, d).start()
            return carry

        lax.fori_loop(0, sp, step, 0)
        HO[mt, half * n:(half + 1) * n, pl.ds(pl.multiple_of(ms * DV, DV), DV)] = OS[half, ms]
        for d in range(sp - 1):
            o_send(half, d).wait()
        for d in range(nx - 1):
            g_send(half, d).start()
        e_send(half).start()

    weights[3].wait()
    width = sp * DV
    for half in range(nl):
        for d in range(nx - 1):
            g_send(half, d).wait()
            h_send(half, d).start()
        e_send(half).wait()
        for d in range(nx - 1):
            h_send(half, d).wait()
        rows = slice(half * n, (half + 1) * n)
        mixed = jnp.zeros((n, cols), F32)
        for t in range(tp):
            mixed = mixed + jnp.dot(
                HO[t, rows, :], WO[t * width:(t + 1) * width, :], preferred_element_type=F32
            )
        residual = X[mt, pl.ds(n + half * n, n), :].astype(F32)
        out[rows, :] = (residual + CO[mt, 4:5, :] * mixed).astype(BF)


def swap_lanes(v):
    quarter = DK // 4
    return jnp.concatenate(
        [
            v[..., quarter:2 * quarter], v[..., :quarter],
            v[..., 3 * quarter:], v[..., 2 * quarter:3 * quarter],
        ],
        axis=-1,
    )


def fused(
    sp, tp, latent, context, conditions, mod_weight, norm_gain, w_query, w_key, w_value,
    query_gain, key_gain, lambdas, out_gain, w_out,
):
    tok, cols = latent.shape
    n = context.shape[0]
    nl = tok // n
    activated = jax.nn.silu(conditions).astype(BF).astype(F32)
    weight = mod_weight.astype(F32)
    part = jnp.concatenate(
        [jnp.sum(weight * activated[c][:, None, None], axis=0) for c in range(2)]
        + [jnp.zeros((2, cols), F32)],
        axis=0,
    )
    positions = lax.axis_index("sp") * tok + jnp.arange(tok, dtype=jnp.int32)
    quarter = DK // 4
    inverse = 10000.0 ** (-4.0 * jnp.arange(quarter, dtype=F32) / DK)
    row_angle = (positions // GRID_W).astype(F32)[:, None] * inverse
    column_angle = (positions % GRID_W).astype(F32)[:, None] * inverse
    cosine = jnp.concatenate([jnp.cos(row_angle)] * 2 + [jnp.cos(column_angle)] * 2, axis=1)
    rs, cs = jnp.sin(row_angle), jnp.sin(column_angle)
    sine = jnp.concatenate([-rs, rs, -cs, cs], axis=1)
    factor = DK ** (-0.5) * math.log2(math.e)

    def pair(g, scale):
        c = cosine * (g * scale)
        s = sine * (swap_lanes(g) * scale)
        return jnp.concatenate([c, c], axis=1), jnp.concatenate([s, s], axis=1)

    qc, qs = pair(query_gain, factor)
    kc, ks = pair(key_gain, 1.0)
    ckg = jnp.concatenate([key_gain, key_gain])[None]
    lam = jnp.broadcast_to(
        lax.dynamic_slice_in_dim(lambdas, lax.axis_index("sp"), 1)[None], (1, DV)
    )
    which = jnp.arange(2 * DK) // DK
    ones_bd = (which[:, None] == which[None]).astype(BF)
    nx = tp // 2
    any_ = pl.BlockSpec(memory_space=pl.ANY)
    vm = pl.BlockSpec(memory_space=pltpu.VMEM)
    dma = pltpu.SemaphoreType.DMA
    kdim, wcols = w_query.shape
    nk = sp * (nl + 1)
    return pl.pallas_call(
        functools.partial(fused_kernel, sp, tp),
        out_shape=jax.ShapeDtypeStruct((tok, cols), BF),
        in_specs=[any_, any_, vm, vm, any_, any_, any_, any_] + [vm] * 8,
        out_specs=vm,
        scratch_shapes=[
            pltpu.VMEM((tp, n + tok, cols), BF),
            pltpu.VMEM((sp, 8, cols), F32),
            pltpu.VMEM((tp, 8, cols), F32),
            pltpu.VMEM((kdim, wcols), BF),
            pltpu.VMEM((kdim, wcols), BF),
            pltpu.VMEM((kdim, wcols), BF),
            pltpu.VMEM(w_out.shape, BF),
            pltpu.VMEM((n, kdim), BF),
            pltpu.VMEM((sp, nl, n, 3 * DV), BF),
            pltpu.VMEM((sp, n, 2 * DV), BF),
            pltpu.VMEM((sp, nl, n, 3 * DV), BF),
            pltpu.VMEM((sp, n, 2 * DV), BF),
            pltpu.VMEM((nk, n, DV), BF),
            pltpu.VMEM((nk, n, 2 * DV), BF),
            pltpu.VMEM((nk, 2 * n, n), F32),
            pltpu.VMEM((nl, sp, n, DV), BF),
            pltpu.VMEM((tp, tok, sp * DV), BF),
            dma((nl + 1,)),
            dma((4,)),
            dma((nl + 1, nx - 1)), dma((nl + 1, nx - 1)),
            dma((nl + 1,)), dma((nl + 1,)),
            dma((nl + 1, nx - 1)), dma((nl + 1, nx - 1)),
            dma((sp - 1,)), dma((sp - 1,)),
            dma((tp - 1,)), dma((tp - 1,)),
            dma((nl + 1, sp - 1)), dma((nl + 1, sp - 1)),
            dma((nl, sp - 1)), dma((nl, sp - 1)),
            dma((nl, nx - 1)), dma((nl, nx - 1)),
            dma((nl,)), dma((nl,)),
            dma((nl, nx - 1)), dma((nl, nx - 1)),
        ],
        compiler_params=pltpu.CompilerParams(
            collective_id=0, has_side_effects=True, vmem_limit_bytes=60 * 1024 * 1024
        ),
    )(
        latent, context, part, norm_gain[None], w_query, w_key, w_value, w_out,
        qc, qs, kc, ks, ckg, lam, out_gain[None], ones_bd,
    )


def local(sp, tp, *arguments):
    latent, context, lambdas = arguments[0], arguments[1], arguments[10]
    rows = context.shape[0]
    fits = (
        lambdas.shape[0] == sp and sp > 1 and tp % 2 == 0 and tp > 2
        and latent.shape[0] % rows == 0 and rows % 128 == 0 and rows <= 256
        and latent.shape[0] <= 2 * rows and latent.shape[1] % 128 == 0
        and latent.shape[1] <= 1024 and tp <= 4
    )
    if fits:
        return fused(sp, tp, *arguments)
    return plain(*arguments)


def solution(mesh):
    in_specs = (
        P(("grp", "sp"), "tp"),
        P(("grp", "sp"), "tp"),
        P("grp", "sp"),
        P("sp", None, "tp"),
        P("tp"),
        P(None, "tp"),
        P(None, "tp"),
        P(None, "tp"),
        P(),
        P(),
        P("tp"),
        P(),
        P(None, "tp"),
    )
    out_specs = P(("grp", "sp"), "tp")
    body = functools.partial(local, mesh.shape["sp"], mesh.shape["tp"])
    return jax.shard_map(body, mesh=mesh, in_specs=in_specs, out_specs=out_specs, check_vma=False)
```

```python
import functools
import math

import jax
import jax.numpy as jnp
import numpy as np
from jax import lax
from jax.experimental import pallas as pl
from jax.experimental.pallas import tpu as pltpu
from jax.sharding import PartitionSpec as P

DK = 64
DV = 128
GRID_W = 64


epsilon = 1e-06


def turn_half(halves, angles):
    quarter = halves.shape[-1] // 2
    cosine = jnp.cos(angles)[:, None, None, :]
    sine_part = jnp.sin(angles)[:, None, None, :]
    first_part = halves[..., :quarter]
    second = halves[..., quarter:]
    return jnp.concatenate(
        [first_part * cosine - second * sine_part, first_part * sine_part + second * cosine],
        axis=-1,
    )


def rotate(features, positions):
    half_width = features.shape[-1] // 2
    quarter = half_width // 2
    inverse = 10000.0 ** (-2.0 * jnp.arange(quarter, dtype=jnp.float32) / half_width)
    grid_row = (positions // GRID_W).astype(jnp.float32)
    grid_column = (positions % GRID_W).astype(jnp.float32)
    return jnp.concatenate(
        [
            turn_half(features[..., :half_width], grid_row[:, None] * inverse),
            turn_half(features[..., half_width:], grid_column[:, None] * inverse),
        ],
        axis=-1,
    )


def head_norm(features, gain_row):
    return (
        features
        * lax.rsqrt(jnp.mean(features * features, axis=-1, keepdims=True) + epsilon)
        * gain_row
    )


def modulate(rows_in, gain_row, shift_row, scale_row):
    floats = rows_in.astype(jnp.float32)
    factor = lax.rsqrt(jnp.mean(floats * floats, axis=1, keepdims=True) + epsilon)
    return (floats * factor * gain_row * (1.0 + scale_row) + shift_row).astype(jnp.bfloat16)


def plain(
    latent,
    context,
    conditions,
    mod_weight,
    norm_gain,
    w_query,
    w_key,
    w_value,
    query_gain,
    key_gain,
    lambdas,
    out_gain,
    w_out,
):
    tok_rows = latent.shape[0]
    ctx_rows = context.shape[0]
    columns = latent.shape[1]
    heads_here = lambdas.shape[0]
    in_rows = mod_weight.shape[0]
    activated = jax.nn.silu(conditions).astype(jnp.bfloat16)
    partial_mod = jnp.dot(
        activated, mod_weight.reshape(in_rows, 3 * columns), preferred_element_type=jnp.float32
    ).reshape(2, 3, columns)
    modulation = lax.psum(partial_mod, "sp")
    lat_floats = latent.astype(jnp.float32)
    full_gain, full_pairs = (
        lax.all_gather(norm_gain, "tp", axis=0, tiled=True),
        lax.all_gather(modulation[:, :2], "tp", axis=2, tiled=True),
    )
    whole_lat, whole_ctx = (
        lax.all_gather(latent, "tp", axis=1, tiled=True),
        lax.all_gather(context, "tp", axis=1, tiled=True),
    )
    hidden = modulate(whole_lat, full_gain, full_pairs[0, 0], full_pairs[0, 1])
    hidden_ctx = modulate(whole_ctx, full_gain, full_pairs[1, 0], full_pairs[1, 1])
    query_raw = jnp.dot(hidden, w_query, preferred_element_type=jnp.float32)
    key_raw = jnp.dot(hidden, w_key, preferred_element_type=jnp.float32)
    value_raw = jnp.dot(hidden, w_value, preferred_element_type=jnp.float32)
    ctx_key_raw = jnp.dot(hidden_ctx, w_key, preferred_element_type=jnp.float32)
    ctx_value_raw = jnp.dot(hidden_ctx, w_value, preferred_element_type=jnp.float32)
    positions = lax.axis_index("sp") * tok_rows + jnp.arange(tok_rows, dtype=jnp.int32)
    queries = rotate(
        head_norm(query_raw.reshape(tok_rows, heads_here, 2, DK), query_gain), positions
    ).astype(jnp.bfloat16)
    lat_keys = (
        rotate(head_norm(key_raw.reshape(tok_rows, heads_here, 2, DK), key_gain), positions)
        .astype(jnp.bfloat16)
        .reshape(tok_rows, heads_here * 2 * DK)
    )
    lat_values = value_raw.astype(jnp.bfloat16)
    ctx_keys = (
        head_norm(ctx_key_raw.reshape(ctx_rows, heads_here, 2, DK), key_gain)
        .astype(jnp.bfloat16)
        .reshape(ctx_rows, heads_here * 2 * DK)
    )
    ctx_values = ctx_value_raw.astype(jnp.bfloat16)
    scaling = DK ** (-0.5)

    def absorb(carried, key_rows, value_rows):
        key_count = key_rows.shape[0]
        key_block = key_rows.reshape(key_count, heads_here, 2, DK)
        value_block = value_rows.reshape(key_count, heads_here, DV)
        running_max, totals, weighted = carried
        scores = (
            jnp.einsum("qhmd,khmd->qhmk", queries, key_block, preferred_element_type=jnp.float32)
            * scaling
        )
        new_max = jnp.maximum(running_max, jnp.max(scores, axis=-1))
        rescale = jnp.exp(running_max - new_max)
        exponent = jnp.exp(scores - new_max[..., None])
        totals = totals * rescale + jnp.sum(exponent, axis=-1)
        weighted = weighted * rescale[..., None] + jnp.einsum(
            "qhmk,khv->qhmv",
            exponent.astype(jnp.bfloat16),
            value_block,
            preferred_element_type=jnp.float32,
        )
        return (new_max, totals, weighted)

    def absorb_rows(carried, key_rows, value_rows):
        key_count = key_rows.shape[0]
        block_rows = math.gcd(key_count, 512)

        def visit_block(block_index, partial_value):
            first_row = block_index * block_rows
            return absorb(
                partial_value,
                lax.dynamic_slice_in_dim(key_rows, first_row, block_rows, 0),
                lax.dynamic_slice_in_dim(value_rows, first_row, block_rows, 0),
            )

        return lax.fori_loop(0, key_count // block_rows, visit_block, carried)

    initial_state = (
        jnp.full((tok_rows, heads_here, 2), -1e30, jnp.float32),
        jnp.zeros((tok_rows, heads_here, 2), jnp.float32),
        jnp.zeros((tok_rows, heads_here, 2, DV), jnp.float32),
    )
    every_ctx_keys, every_ctx_values = (
        lax.all_gather(ctx_keys, "sp", axis=0, tiled=True),
        lax.all_gather(ctx_values, "sp", axis=0, tiled=True),
    )
    carried = absorb_rows(initial_state, every_ctx_keys, every_ctx_values)
    carried = absorb_rows(
        carried,
        lax.all_gather(lat_keys, "sp", axis=0, tiled=True),
        lax.all_gather(lat_values, "sp", axis=0, tiled=True),
    )
    running_max, totals, weighted = carried
    attended = (
        weighted[:, :, 0] / totals[:, :, 0, None]
        - lambdas[None, :, None] * weighted[:, :, 1] / totals[:, :, 1, None]
    )
    head_out = head_norm(attended, out_gain).astype(jnp.bfloat16).reshape(tok_rows, heads_here * DV)
    mixed_rows = jnp.dot(
        lax.all_gather(head_out, "tp", axis=1, tiled=True),
        w_out,
        preferred_element_type=jnp.float32,
    )
    return (lat_floats + modulation[0, 2] * mixed_rows).astype(jnp.bfloat16)


MESH = pl.DeviceIdType.MESH
BF = jnp.bfloat16
F32 = jnp.float32


def fused_kernel(
    sp, tp, lat, ctx, part, gain, wq_h, wk_h, wv_h, wo_h, qg, kg, rcos, rsin, ccos, csin, lambdas, og,
    out, X, PA, CO, WQ, WK, WV, WO, H, SL, SC, RL, RC, KX, VX, SS, AC, PK, OS, HO,
    loc_sem, w_sem, xs, xr, ds, dr, fs, fr, ps, pr, cs, cr, zs, zr, os_, or_, gs, gr, es, er, hs, hr,
):
    ms = lax.axis_index("sp")
    mt = lax.axis_index("tp")
    nx = tp // 2
    core = lax.rem(mt, 2)
    base = mt - core
    mate = base + 1 - core
    xp = [lax.rem(base + 2 * d, tp) + core for d in range(1, nx)]
    xq = [lax.rem(base + tp - 2 * d, tp) + core for d in range(1, nx)]
    xqm = [lax.rem(base + tp - 2 * d, tp) + 1 - core for d in range(1, nx)]
    zp = [lax.rem(ms + d, sp) for d in range(1, sp)]
    zq = [lax.rem(ms + sp - d, sp) for d in range(1, sp)]
    tpn = [lax.rem(mt + d, tp) for d in range(1, tp)]
    tpq = [lax.rem(mt + tp - d, tp) for d in range(1, tp)]
    n = ctx.shape[0]
    cols = lat.shape[1]
    nl = lat.shape[0] // n

    barrier = pltpu.get_barrier_semaphore()
    for p in zp:
        pl.semaphore_signal(barrier, inc=1, device_id={"sp": p}, device_id_type=MESH)
    for p in tpn:
        pl.semaphore_signal(barrier, inc=1, device_id={"tp": p}, device_id_type=MESH)

    def local_in(c):
        src = ctx if c == 0 else lat.at[pl.ds((c - 1) * n, n)]
        return pltpu.make_async_copy(src, X.at[mt, pl.ds(c * n, n)], loc_sem.at[c])

    for c in range(nl + 1):
        local_in(c).start()
    weights = [
        pltpu.make_async_copy(a, b, w_sem.at[i])
        for i, (a, b) in enumerate(((wk_h, WK), (wv_h, WV), (wq_h, WQ), (wo_h, WO)))
    ]
    for w in weights:
        w.start()
    pl.semaphore_wait(barrier, (sp - 1) + (tp - 1))

    def remote(src, dst, ssem, rsem, where):
        return pltpu.make_async_remote_copy(
            src_ref=src, dst_ref=dst, send_sem=ssem, recv_sem=rsem,
            device_id=where, device_id_type=MESH,
        )

    def source(c):
        return ctx if c == 0 else lat.at[pl.ds((c - 1) * n, n)]

    def x_send(c, d):
        return remote(source(c), X.at[mt, pl.ds(c * n, n)], xs.at[c, d], xr.at[c, d], {"tp": xp[d]})

    def d_send(c):
        return remote(source(c), X.at[mt, pl.ds(c * n, n)], ds.at[c], dr.at[c], {"tp": mate})

    def p_send(d):
        return remote(part, PA.at[ms], ps.at[d], pr.at[d], {"sp": zp[d]})

    def c_send(d):
        return remote(CO.at[mt], CO.at[mt], cs.at[d], cr.at[d], {"tp": tpn[d]})

    for d in range(sp - 1):
        p_send(d).start()
    for d in range(nx - 1):
        x_send(0, d).start()
    for c in range(nl + 1):
        d_send(c).start()

    PA[ms] = part[...]
    for d in range(sp - 1):
        p_send(d).wait()
    total = PA[0]
    for s in range(1, sp):
        total = total + PA[s]
    CO[mt, 0:1, :] = gain[...] * (1.0 + total[1:2])
    CO[mt, 1:2, :] = total[0:1]
    CO[mt, 2:3, :] = gain[...] * (1.0 + total[4:5])
    CO[mt, 3:4, :] = total[3:4]
    CO[mt, 4:5, :] = total[2:3]
    CO[mt, 5:8, :] = jnp.zeros((3, cols), F32)
    for d in range(tp - 1):
        c_send(d).start()
    for c in range(1, nl + 1):
        for d in range(nx - 1):
            x_send(c, d).start()
    for d in range(tp - 1):
        c_send(d).wait()

    lane = lax.broadcasted_iota(jnp.int32, (n, 2 * DK), 1)
    low = lax.rem(lane, DK // 2) < DK // 4
    by_row = lax.rem(lane[:GRID_W], DK) < DK // 2
    bd_row = lax.broadcasted_iota(jnp.int32, (2 * DK, 2 * DK), 0) < DK
    bd_col = lax.broadcasted_iota(jnp.int32, (2 * DK, 2 * DK), 1) < DK
    ones_bd = jnp.where(bd_row == bd_col, 1.0, 0.0).astype(BF)

    def swapped(v):
        where = low[:v.shape[0]]
        return jnp.where(where, pltpu.roll(v, 2 * DK - DK // 4, 1), pltpu.roll(v, DK // 4, 1))

    def gains(ref, scale):
        g = jnp.concatenate([ref[...], ref[...]], axis=1) * scale
        return g, swapped(jnp.broadcast_to(g, (8, 2 * DK)))[0:1]

    q_gain, q_swap = gains(qg, DK ** (-0.5) * math.log2(math.e))
    k_gain, k_swap = gains(kg, 1.0)
    heads_lane = lax.broadcasted_iota(jnp.int32, lambdas.shape, 1)
    lam = jnp.sum(jnp.where(heads_lane == ms, lambdas[...], 0.0), axis=1, keepdims=True)

    def table(row_ref, col_ref, c):
        start = ms * (lat.shape[0] // GRID_W) + (c - 1) * (n // GRID_W)
        return jnp.concatenate(
            [
                jnp.where(by_row, row_ref[pl.ds(start + r, 1), :], col_ref[...])
                for r in range(n // GRID_W)
            ],
            axis=0,
        )

    def f_send(c, d):
        ref = X.at[xq[d], pl.ds(c * n, n)]
        return remote(ref, ref, fs.at[c, d], fr.at[c, d], {"tp": mate})

    def z_send(c, d):
        if c == 0:
            return remote(SC.at[zp[d]], RC.at[ms], zs.at[c, d], zr.at[c, d], {"sp": zp[d]})
        return remote(
            SL.at[zp[d], c - 1], RL.at[ms, c - 1], zs.at[c, d], zr.at[c, d], {"sp": zp[d]}
        )

    def normed(v):
        square = (v * v).astype(BF)
        mean = jnp.dot(square, ones_bd, preferred_element_type=F32)
        return v * lax.rsqrt(mean * (1.0 / DK) + epsilon)

    def turned(v, ctab, stab):
        w = normed(v)
        return (w * ctab + swapped(w) * stab).astype(BF)

    for c in range(nl + 1):
        rows = pl.ds(c * n, n)
        local_in(c).wait()
        for d in range(nx - 1):
            x_send(c, d).wait()
            f_send(c, d).start()
        d_send(c).wait()
        for d in range(nx - 1):
            f_send(c, d).wait()
        ss = jnp.zeros((n, 1), F32)
        for t in range(tp):
            f = X[t, rows, :].astype(F32)
            ss = ss + jnp.sum(f * f, axis=1, keepdims=True)
        factor = lax.rsqrt(ss * (1.0 / (tp * cols)) + epsilon)
        r0 = 2 if c == 0 else 0
        for t in range(tp):
            f = X[t, rows, :].astype(F32)
            co = CO[t]
            H[:, t * cols:(t + 1) * cols] = (
                f * factor * co[r0:r0 + 1] + co[r0 + 1:r0 + 2]
            ).astype(BF)
        if c == 0:
            weights[0].wait()
            weights[1].wait()
        if c == 1:
            weights[2].wait()
        off = 0 if c == 0 else DV
        if c > 0:
            cosine, sine = table(rcos, ccos, c), table(rsin, csin, c)
            qc, qs = cosine * q_gain, sine * q_swap
            kc, ks = cosine * k_gain, sine * k_swap
            raw = jnp.dot(H[...], WQ[...], preferred_element_type=F32)
            for z in range(sp):
                SL[z, c - 1, :, 0:DV] = turned(raw[:, z * DV:(z + 1) * DV], qc, qs)
        raw = jnp.dot(H[...], WK[...], preferred_element_type=F32)
        for z in range(sp):
            piece = raw[:, z * DV:(z + 1) * DV]
            if c == 0:
                SC[z, :, 0:DV] = (normed(piece) * k_gain).astype(BF)
            else:
                SL[z, c - 1, :, DV:2 * DV] = turned(piece, kc, ks)
        raw = jnp.dot(H[...], WV[...], preferred_element_type=F32)
        for z in range(sp):
            piece = raw[:, z * DV:(z + 1) * DV].astype(BF)
            if c == 0:
                SC[z, :, DV:2 * DV] = piece
            else:
                SL[z, c - 1, :, 2 * DV:3 * DV] = piece
        for d in range(sp - 1):
            z_send(c, d).start()
        if c == 0:
            RC[ms] = SC[ms]
        else:
            RL[ms, c - 1] = SL[ms, c - 1]

    def take(c):
        for d in range(sp - 1):
            z_send(c, d).wait()
        for s in range(sp):
            kb = c * sp + s
            if c == 0:
                KX[kb] = RC[s, :, 0:DV]
                VX[kb, :, 0:DV] = RC[s, :, DV:2 * DV]
            else:
                KX[kb] = RL[s, c - 1, :, DV:2 * DV]
                VX[kb, :, 0:DV] = RL[s, c - 1, :, 2 * DV:3 * DV]
            VX[kb, :, DV:2 * DV] = jnp.ones((n, DV), BF)

    first = lane < DK

    def o_send(half, d):
        return remote(
            OS.at[half, zp[d]],
            HO.at[mt, pl.ds(half * n, n), pl.ds(pl.multiple_of(ms * DV, DV), DV)],
            os_.at[half, d], or_.at[half, d], {"sp": zp[d]},
        )

    def g_send(half, d):
        ref = HO.at[mt, pl.ds(half * n, n)]
        return remote(ref, ref, gs.at[half, d], gr.at[half, d], {"tp": xp[d]})

    def e_send(half):
        ref = HO.at[mt, pl.ds(half * n, n)]
        return remote(ref, ref, es.at[half], er.at[half], {"tp": mate})

    def h_send(half, d):
        ref = HO.at[xq[d], pl.ds(half * n, n)]
        return remote(ref, ref, hs.at[half, d], hr.at[half, d], {"tp": mate})

    def stacked(z, half):
        q = RL[z, half, :, 0:DV]
        zero = jnp.zeros_like(q)
        return jnp.concatenate([jnp.where(first, q, zero), jnp.where(first, zero, q)], axis=0)

    def merge(old, new):
        peak = jnp.maximum(old[0], new[0])
        return peak, old[1] * jnp.exp2(old[0] - peak) + new[1] * jnp.exp2(new[0] - peak)

    def attend(zs_here, half, groups, states):
        queries = [stacked(z, half) for z in zs_here]
        stages = [(i, g) for i in range(len(zs_here)) for g in groups]
        peaks = {}

        def score(k, j):
            i, g = stages[k]
            s = lax.dot_general(
                queries[i], KX[g * sp + j], (((1,), (1,)), ((), ())), preferred_element_type=F32
            )
            SS[k * sp + j] = s
            for m in range(n // 128):
                piece = s[:, m * 128:(m + 1) * 128]
                peaks[k] = piece if k not in peaks else jnp.maximum(peaks[k], piece)

        for j in range(sp):
            score(0, j)
        for k, (i, g) in enumerate(stages):
            peak = jnp.max(peaks[k], axis=1, keepdims=True)
            acc = None
            for j in range(sp):
                p = jnp.exp2(SS[k * sp + j] - peak).astype(BF)
                term = jnp.dot(p, VX[g * sp + j], preferred_element_type=F32)
                acc = term if acc is None else acc + term
                if k + 1 < len(stages):
                    score(k + 1, j)
            states[i] = (peak, acc) if states[i] is None else merge(states[i], (peak, acc))
        return states

    def finish(state):
        acc = state[1]
        o = acc[:, :DV] / acc[:, DV:]
        a = o[:n] - lam * o[n:]
        a = a * lax.rsqrt(jnp.mean(a * a, axis=1, keepdims=True) + epsilon) * og[...]
        return a.astype(BF)

    per = 2 if sp % 2 == 0 else 1

    def places(i):
        return [lax.rem(ms + 1 + i * per + e, sp) for e in range(per)]

    early = nl - 1
    for c in range(nl):
        take(c)

    def ahead(i, carry):
        here = places(i)
        for z, (peak, acc) in zip(here, attend(here, 0, range(nl), [None] * per)):
            AC[z] = acc
            PK[z] = jnp.broadcast_to(peak, (2 * n, DV))
        return carry

    if early:
        lax.fori_loop(0, sp // per, ahead, 0)
    take(nl)

    for half in range(nl):
        def step(i, carry):
            here = places(i)
            if early and half == 0:
                states = [(PK[z][:, 0:1], AC[z]) for z in here]
                states = attend(here, half, [nl], states)
            else:
                states = attend(here, half, range(nl + 1), [None] * per)
            for e, z in enumerate(here):
                OS[half, z] = finish(states[e])
                for d in range(sp - 1):
                    if d % per == e:
                        @pl.when(i == d // per)
                        def _():
                            o_send(half, d).start()
            return carry

        lax.fori_loop(0, sp // per, step, 0)
        HO[mt, half * n:(half + 1) * n, pl.ds(pl.multiple_of(ms * DV, DV), DV)] = OS[half, ms]
        for d in range(sp - 1):
            o_send(half, d).wait()
        for d in range(nx - 1):
            g_send(half, d).start()
        e_send(half).start()

    weights[3].wait()
    width = sp * DV
    for half in range(nl):
        for d in range(nx - 1):
            g_send(half, d).wait()
            h_send(half, d).start()
        e_send(half).wait()
        for d in range(nx - 1):
            h_send(half, d).wait()
        rows = slice(half * n, (half + 1) * n)
        mixed = jnp.zeros((n, cols), F32)
        for t in range(tp):
            mixed = mixed + jnp.dot(
                HO[t, rows, :], WO[t * width:(t + 1) * width, :], preferred_element_type=F32
            )
        residual = X[mt, pl.ds(n + half * n, n), :].astype(F32)
        out[rows, :] = (residual + CO[mt, 4:5, :] * mixed).astype(BF)


def fused(
    sp, tp, latent, context, conditions, mod_weight, norm_gain, w_query, w_key, w_value,
    query_gain, key_gain, lambdas, out_gain, w_out,
):
    tok, cols = latent.shape
    n = context.shape[0]
    nl = tok // n
    activated = jax.nn.silu(conditions).astype(BF).astype(F32)
    weight = mod_weight.astype(F32)
    part = jnp.concatenate(
        [jnp.sum(weight * activated[c][:, None, None], axis=0) for c in range(2)]
        + [jnp.zeros((2, cols), F32)],
        axis=0,
    )
    inverse = 10000.0 ** (-4.0 * np.arange(DK // 4) / DK)
    sign = np.where(np.arange(2 * DK) % (DK // 2) < DK // 4, -1.0, 1.0)

    def trig(count):
        angles = np.arange(count)[:, None] * np.tile(inverse, 8)[None]
        return (
            jnp.asarray(np.cos(angles).astype(np.float32)),
            jnp.asarray((np.sin(angles) * sign).astype(np.float32)),
        )

    rcos, rsin = trig(sp * tok // GRID_W)
    ccos, csin = trig(GRID_W)
    nx = tp // 2
    any_ = pl.BlockSpec(memory_space=pl.ANY)
    vm = pl.BlockSpec(memory_space=pltpu.VMEM)
    dma = pltpu.SemaphoreType.DMA
    kdim, wcols = w_query.shape
    nk = sp * (nl + 1)
    return pl.pallas_call(
        functools.partial(fused_kernel, sp, tp),
        out_shape=jax.ShapeDtypeStruct((tok, cols), BF),
        in_specs=[any_, any_, vm, vm, any_, any_, any_, any_] + [vm] * 8,
        out_specs=vm,
        scratch_shapes=[
            pltpu.VMEM((tp, n + tok, cols), BF),
            pltpu.VMEM((sp, 8, cols), F32),
            pltpu.VMEM((tp, 8, cols), F32),
            pltpu.VMEM((kdim, wcols), BF),
            pltpu.VMEM((kdim, wcols), BF),
            pltpu.VMEM((kdim, wcols), BF),
            pltpu.VMEM(w_out.shape, BF),
            pltpu.VMEM((n, kdim), BF),
            pltpu.VMEM((sp, nl, n, 3 * DV), BF),
            pltpu.VMEM((sp, n, 2 * DV), BF),
            pltpu.VMEM((sp, nl, n, 3 * DV), BF),
            pltpu.VMEM((sp, n, 2 * DV), BF),
            pltpu.VMEM((nk, n, DV), BF),
            pltpu.VMEM((nk, n, 2 * DV), BF),
            pltpu.VMEM((2 * nk, 2 * n, n), F32),
            pltpu.VMEM((sp, 2 * n, 2 * DV), F32),
            pltpu.VMEM((sp, 2 * n, DV), F32),
            pltpu.VMEM((nl, sp, n, DV), BF),
            pltpu.VMEM((tp, tok, sp * DV), BF),
            dma((nl + 1,)),
            dma((4,)),
            dma((nl + 1, nx - 1)), dma((nl + 1, nx - 1)),
            dma((nl + 1,)), dma((nl + 1,)),
            dma((nl + 1, nx - 1)), dma((nl + 1, nx - 1)),
            dma((sp - 1,)), dma((sp - 1,)),
            dma((tp - 1,)), dma((tp - 1,)),
            dma((nl + 1, sp - 1)), dma((nl + 1, sp - 1)),
            dma((nl, sp - 1)), dma((nl, sp - 1)),
            dma((nl, nx - 1)), dma((nl, nx - 1)),
            dma((nl,)), dma((nl,)),
            dma((nl, nx - 1)), dma((nl, nx - 1)),
        ],
        compiler_params=pltpu.CompilerParams(
            collective_id=0, has_side_effects=True, vmem_limit_bytes=60 * 1024 * 1024
        ),
    )(
        latent, context, part, norm_gain[None], w_query, w_key, w_value, w_out,
        query_gain[None], key_gain[None], rcos, rsin, ccos, csin, lambdas[None], out_gain[None],
    )


def local(sp, tp, *arguments):
    latent, context, lambdas = arguments[0], arguments[1], arguments[10]
    rows = context.shape[0]
    fits = (
        lambdas.shape[0] == sp and sp > 1 and tp % 2 == 0 and tp > 2
        and latent.shape[0] % rows == 0 and rows % 128 == 0 and rows <= 256 and rows % GRID_W == 0
        and latent.shape[0] <= 2 * rows and latent.shape[1] % 128 == 0
        and latent.shape[1] <= 1024 and tp <= 4
    )
    if fits:
        return fused(sp, tp, *arguments)
    return plain(*arguments)


def solution(mesh):
    in_specs = (
        P(("grp", "sp"), "tp"),
        P(("grp", "sp"), "tp"),
        P("grp", "sp"),
        P("sp", None, "tp"),
        P("tp"),
        P(None, "tp"),
        P(None, "tp"),
        P(None, "tp"),
        P(),
        P(),
        P("tp"),
        P(),
        P(None, "tp"),
    )
    out_specs = P(("grp", "sp"), "tp")
    body = functools.partial(local, mesh.shape["sp"], mesh.shape["tp"])
    return jax.shard_map(body, mesh=mesh, in_specs=in_specs, out_specs=out_specs, check_vma=False)
```
